32 devices in a mesh: sp: 8 (over z, x), tp: 4 (over y, core).
Axes of the slice: x: 2, y: 2, z: 4, core: 2. Of those that a mesh axis runs over, the one named last changes fastest.
Arguments:
- q_first: bfloat16 [1536, 512], P('sp', 'tp'), may hold values from -6 to 6
- k_first: bfloat16 [1536, 512], P('sp', 'tp'), may hold values from -6 to 6
- q_second: bfloat16 [1536, 512], P('sp', 'tp'), may hold values from -6 to 6
- k_second: bfloat16 [1536, 512], P('sp', 'tp'), may hold values from -6 to 6
- values: bfloat16 [1536, 1024], P('sp', 'tp'), may hold values from -6 to 6
- lambdas: float32 [8], P('tp'), may hold values from 0.3 to 0.8
- head_gain: float32 [128], replicated, may hold values from 0.1 to 1.9
- out_weight: bfloat16 [1024, 2048], P('tp'), may hold values from -0.1875 to 0.1875
- residual_in: bfloat16 [1536, 2048], P('sp'), may hold values from -6 to 6
- mix_gain: float32 [2048], replicated, may hold values from 0.1 to 1.9
- gate_weight: bfloat16 [2048, 5632], P('sp', 'tp'), may hold values from -0.125 to 0.125
- up_weight: bfloat16 [2048, 5632], P('sp', 'tp'), may hold values from -0.125 to 0.125
- gate_taps: float32 [3, 5632], P(None, 'tp'), may hold values from -3.5 to 3.5
- up_taps: float32 [3, 5632], P(None, 'tp'), may hold values from -3.5 to 3.5
- down_weight: bfloat16 [5632, 2048], P('tp'), may hold values from -0.078125 to 0.078125
Outputs:
- mixed: bfloat16 [1536, 2048], P(('sp', 'tp'))
The draws below stay inside these ranges and needn't reach their ends.
All inputs are finite; a program needn't handle non-finite values.
Results may differ from the reference program's by a relative error of at most 0.017.
Values may be sent and summed in bfloat16 or wider, within the bound.
A program may use at most 128 MiB of HBM per device.

```python
import math
import jax
import jax.numpy as jnp
from jax import lax

D = 2048
HEADS = 8
HEAD_DIM = 64
VALUE_DIM = 128
FF = 5632
KERNEL = 3
TOKENS = 1536


def aligned_pair(key):
    shape = (TOKENS, HEADS * HEAD_DIM)
    query_key = jax.random.fold_in(key, 71)
    other_key = jax.random.fold_in(key, 72)
    queries = jnp.clip(1.35 * jax.random.normal(query_key, shape, jnp.float32), -6.0, 6.0)
    keys = jnp.clip(1.35 * jax.random.normal(other_key, shape, jnp.float32), -6.0, 6.0)
    return (queries.astype(jnp.bfloat16), keys.astype(jnp.bfloat16))


def draw_q_first(key, part):
    return aligned_pair(key)[0]


def draw_k_first(key, part):
    return aligned_pair(key)[1]


def shard_levels(own_key, extent, pieces, low, top_value):
    loudness = 1.0
    for position, shards_of in pieces:
        heights = jax.random.uniform(jax.random.fold_in(jax.random.fold_in(own_key, 6), position), (shards_of,), jnp.float32, low / len(pieces), top_value / len(pieces))
        loudness = loudness * jnp.repeat(jnp.exp(heights), extent[position] // shards_of).reshape((-1,) + (1,) * (len(extent) - 1 - position))
    return loudness


def normal_values(key, dims, spread, limit, split=(), kind=jnp.bfloat16):
    entries = spread * jax.random.normal(key, dims, jnp.float32)
    if split:
        entries = entries * shard_levels(key, dims, split, -0.22, 0.18)
    return jnp.clip(entries, -limit, limit).astype(kind)


def setup_inputs(seed: int = 0) -> dict:
    arg_keys = jax.random.split(jax.random.key(seed), 16)
    return {
        "q_first": draw_q_first(jax.random.fold_in(arg_keys[15], 71), 0),
        "k_first": draw_k_first(jax.random.fold_in(arg_keys[15], 71), 0),
        "q_second": normal_values(arg_keys[2], (TOKENS, HEADS * HEAD_DIM), 1.35, 6.0, ((0, 8), (1, 4))),
        "k_second": normal_values(arg_keys[3], (TOKENS, HEADS * HEAD_DIM), 1.35, 6.0, ((0, 8), (1, 4))),
        "values": normal_values(arg_keys[4], (TOKENS, HEADS * VALUE_DIM), 1.0, 6.0, ((0, 8), (1, 4))),
        "lambdas": jnp.clip(0.3 + 0.5 * jax.random.uniform(arg_keys[5], (HEADS,), jnp.float32) ** shard_levels(arg_keys[5], (HEADS,), ((0, 4),), -0.2, 0.2), 0.3, 0.8),
        "head_gain": jnp.clip(1.0 + 0.18 * jax.random.normal(arg_keys[6], (VALUE_DIM,), jnp.float32), 0.1, 1.9),
        "out_weight": normal_values(arg_keys[7], (HEADS * VALUE_DIM, D), (HEADS * VALUE_DIM) ** -0.5, 0.1875, ((0, 4),)),
        "residual_in": normal_values(arg_keys[8], (TOKENS, D), 1.0, 6.0, ((0, 8),)),
        "mix_gain": jnp.clip(1.0 + 0.18 * jax.random.normal(arg_keys[9], (D,), jnp.float32), 0.1, 1.9),
        "gate_weight": normal_values(arg_keys[10], (D, FF), D ** -0.5, 0.125, ((0, 8), (1, 4))),
        "up_weight": normal_values(arg_keys[11], (D, FF), D ** -0.5, 0.125, ((0, 8), (1, 4))),
        "gate_taps": normal_values(arg_keys[12], (KERNEL, FF), KERNEL ** -0.5, 3.5, ((1, 4),), jnp.float32),
        "up_taps": normal_values(arg_keys[13], (KERNEL, FF), KERNEL ** -0.5, 3.5, ((1, 4),), jnp.float32),
        "down_weight": normal_values(arg_keys[14], (FF, D), FF ** -0.5, 0.078125, ((0, 4),)),
    }


norm_eps = 1e-06
far_below = -1e+30

def reference(q_first, k_first, q_second, k_second, values, lambdas, head_gain, out_weight, residual_in, mix_gain, gate_weight, up_weight, gate_taps, up_taps, down_weight):
    total = q_first.shape[0]
    scale = HEAD_DIM ** (-0.5)
    query_a = q_first.astype(jnp.float32).reshape(total, HEADS, HEAD_DIM)
    query_b = q_second.astype(jnp.float32).reshape(total, HEADS, HEAD_DIM)
    keys_a = k_first.astype(jnp.float32).reshape(total, HEADS, HEAD_DIM)
    keys_b = k_second.astype(jnp.float32).reshape(total, HEADS, HEAD_DIM)
    vals = values.astype(jnp.float32).reshape(total, HEADS, VALUE_DIM)
    block_rows = math.gcd(total, 512)
    key_pos = jnp.arange(total, dtype=jnp.int32)

    def weigh(queries, keys, visible):
        scores = jnp.einsum('qhd,khd->hqk', queries, keys, precision=lax.Precision.HIGHEST) * scale
        masked = jnp.where(visible, scores, far_below)
        peak = lax.optimization_barrier(jnp.max(masked, axis=-1, keepdims=True))
        expo = jnp.where(visible, jnp.exp(masked - peak), 0.0)
        totals = lax.optimization_barrier(jnp.sum(expo, axis=-1))
        rounded = expo.astype(jnp.bfloat16).astype(jnp.float32)
        accum = jnp.einsum('hqk,khv->qhv', rounded, vals, precision=lax.Precision.HIGHEST)
        return accum / totals.T[..., None]

    def attend(block_index):
        row_start = (block_index * block_rows).astype(jnp.int32)
        query_pos = row_start + jnp.arange(block_rows, dtype=jnp.int32)
        visible = (key_pos[None, :] <= query_pos[:, None])[None]
        first = weigh(lax.dynamic_slice_in_dim(query_a, row_start, block_rows, 0), keys_a, visible)
        second = weigh(lax.dynamic_slice_in_dim(query_b, row_start, block_rows, 0), keys_b, visible)
        diff_heads = first - lambdas[None, :, None] * second
        normed = diff_heads * lax.rsqrt(lax.optimization_barrier(jnp.mean(diff_heads * diff_heads, axis=-1, keepdims=True)) + norm_eps) * head_gain
        return normed.astype(jnp.bfloat16).reshape(block_rows, HEADS * VALUE_DIM)
    head_out = lax.map(attend, jnp.arange(total // block_rows, dtype=jnp.int32)).reshape(total, HEADS * VALUE_DIM)
    attended = jnp.dot(head_out, out_weight, preferred_element_type=jnp.float32)
    stream = residual_in.astype(jnp.float32) + attended
    ffn_in = (stream * lax.rsqrt(lax.optimization_barrier(jnp.mean(stream * stream, axis=-1, keepdims=True)) + norm_eps) * mix_gain).astype(jnp.bfloat16)
    gate_pre = jnp.dot(ffn_in, gate_weight, preferred_element_type=jnp.float32).astype(jnp.bfloat16)
    up_pre = jnp.dot(ffn_in, up_weight, preferred_element_type=jnp.float32).astype(jnp.bfloat16)

    def convolve(projected, taps):
        padded = jnp.pad(projected.astype(jnp.float32), ((KERNEL - 1, 0), (0, 0)))
        result = taps[0][None, :] * padded[0:total]
        for offset in range(1, KERNEL):
            result = result + taps[offset][None, :] * padded[offset:offset + total]
        return result
    gate_conv = convolve(gate_pre, gate_taps)
    up_conv = convolve(up_pre, up_taps)
    hidden = (jax.nn.silu(gate_conv) * up_conv).astype(jnp.bfloat16)
    return (stream + jnp.dot(hidden, down_weight, preferred_element_type=jnp.float32)).astype(jnp.bfloat16)
```

```python
import functools

import jax
import jax.numpy as jnp
from jax import lax
from jax.experimental import pallas as pl
from jax.experimental.pallas import tpu as pltpu
from jax.sharding import PartitionSpec as P

norm_eps = 1e-06
far_below = -1e30
halo = 16
lanes = 2
f32 = jnp.float32
bf16 = jnp.bfloat16


def rms_scale(field, gain):
    return field * lax.rsqrt(jnp.mean(field * field, axis=-1, keepdims=True) + norm_eps) * gain


def layer(
    sp_count,
    tp_count,
    q_a,
    k_a,
    q_b,
    k_b,
    vals,
    lambdas,
    head_gain,
    out_weight,
    residual,
    mix_gain,
    gate_weight,
    up_weight,
    gate_taps,
    up_taps,
    down_weight,
    out,
    kv,
    w,
    down,
    out_w,
    res,
    heads,
    part_out,
    part_in,
    stream,
    ffn,
    acc,
    hidden,
    last_out,
    last_in,
    local,
    kvz_send,
    kvz_recv,
    kvx_send,
    kvx_recv,
    wz_send,
    wz_recv,
    wx_send,
    wx_recv,
    rs_send,
    rs_recv,
    ag_send,
    ag_recv,
    halo_send,
    halo_recv,
    last_send,
    last_recv,
):
    s = lax.axis_index("sp")
    t = lax.axis_index("tp")
    x = lax.rem(s, lanes)
    z = s // lanes
    lines = sp_count // lanes
    mate = z * lanes + (1 - x)
    rows = q_a.shape[0]
    key_width = q_a.shape[1]
    value_width = vals.shape[1]
    head_count = lambdas.shape[0]
    head_dim = key_width // head_count
    value_dim = value_width // head_count
    part = rows // tp_count
    width = out.shape[1]
    w_rows = gate_weight.shape[0]
    ff = gate_weight.shape[1]
    taps = gate_taps.shape[0]

    def remote(src, dst, send, recv, sp, tp):
        return pltpu.make_async_remote_copy(
            src_ref=src,
            dst_ref=dst,
            send_sem=send,
            recv_sem=recv,
            device_id=(sp, tp),
            device_id_type=pl.DeviceIdType.MESH,
        )

    def kv_block(block):
        return kv.at[pl.ds(pl.multiple_of(block * rows, 16), rows)]

    def w_block(c, block):
        return w.at[c, pl.ds(pl.multiple_of(block * w_rows, 16), w_rows)]

    own = pl.ds(pl.multiple_of(s * rows, 16), rows)
    kv_loads = (
        pltpu.make_async_copy(k_a, kv.at[own, pl.ds(0, key_width)], local.at[0]),
        pltpu.make_async_copy(k_b, kv.at[own, pl.ds(key_width, key_width)], local.at[1]),
        pltpu.make_async_copy(vals, kv.at[own, pl.ds(2 * key_width, value_width)], local.at[2]),
    )
    w_loads = (
        pltpu.make_async_copy(gate_weight, w_block(0, s), local.at[3]),
        pltpu.make_async_copy(up_weight, w_block(1, s), local.at[4]),
    )
    out_load = pltpu.make_async_copy(out_weight, out_w, local.at[5])
    res_load = pltpu.make_async_copy(
        residual.at[pl.ds(pl.multiple_of(t * part, 16), part)], res, local.at[6]
    )
    down_load = pltpu.make_async_copy(down_weight, down, local.at[7])
    for load in kv_loads + w_loads + (out_load, res_load, down_load):
        load.start()

    barrier = pltpu.get_barrier_semaphore()

    @pl.loop(1, sp_count)
    def _(i):
        pl.semaphore_signal(
            barrier,
            inc=1,
            device_id=(lax.rem(s + i, sp_count), t),
            device_id_type=pl.DeviceIdType.MESH,
        )

    @pl.loop(1, tp_count)
    def _(i):
        pl.semaphore_signal(
            barrier,
            inc=1,
            device_id=(s, lax.rem(t + i, tp_count)),
            device_id_type=pl.DeviceIdType.MESH,
        )

    pl.semaphore_wait(barrier, sp_count + tp_count - 2)

    def kvz(line, to, index):
        block = kv_block(line * lanes + x)
        return remote(block, block, kvz_send.at[index], kvz_recv.at[line], to * lanes + x, t)

    def kvx(line, lane):
        block = kv_block(line * lanes + lane)
        return remote(block, block, kvx_send.at[line], kvx_recv.at[line], mate, t)

    def wz(c, line, to, index):
        block = w_block(c, line * lanes + x)
        return remote(block, block, wz_send.at[c, index], wz_recv.at[c, line], to * lanes + x, t)

    def wx(c, line, lane):
        block = w_block(c, line * lanes + lane)
        return remote(block, block, wx_send.at[c, line], wx_recv.at[c, line], mate, t)

    for load in kv_loads:
        load.wait()

    @pl.loop(z + 1, lines)
    def _(to):
        kvz(z, to, to).start()

    kvx(z, x).start()
    for load in w_loads:
        load.wait()

    @pl.loop(1, lines)
    def _(i):
        to = lax.rem(z + lines - i, lines)
        for c in range(2):
            wz(c, z, to, to).start()

    @pl.loop(0, z)
    def _(i):
        line = z - 1 - i
        kvz(line, mate // lanes, line).wait_recv()
        kvx(line, x).start()

    for c in range(2):
        wx(c, z, x).start()

    scale = head_dim**-0.5
    column = lax.broadcasted_iota(jnp.int32, (rows, key_width), 1) // head_dim
    queries = [
        jnp.where(column == h, q[...], jnp.zeros((), bf16))
        for q in (q_a, q_b)
        for h in range(head_count)
    ]
    span = lanes * rows
    query_pos = s * rows + lax.broadcasted_iota(jnp.int32, (rows, span), 0)
    key_step = lax.broadcasted_iota(jnp.int32, (rows, span), 1)

    def attend(i, state):
        line = z - i
        kvx(line, 1 - x).wait_recv()
        keys_at = pl.ds(pl.multiple_of(line * span, 16), span)
        visible = line * span + key_step <= query_pos
        following = []
        for m in range(2):
            keys = kv[keys_at, pl.ds(m * key_width, key_width)]
            for h in range(head_count):
                peak, total, sums = state[m * head_count + h]
                value = kv[keys_at, pl.ds(2 * key_width + h * value_dim, value_dim)]
                scores = (
                    lax.dot_general(
                        queries[m * head_count + h],
                        keys,
                        (((1,), (1,)), ((), ())),
                        preferred_element_type=f32,
                    )
                    * scale
                )
                scores = jnp.where(visible, scores, far_below)
                new_peak = jnp.maximum(peak, jnp.max(scores, axis=-1, keepdims=True))
                fade = jnp.exp(peak - new_peak)
                expo = jnp.exp(scores - new_peak)
                total = total * fade + jnp.sum(expo, axis=-1, keepdims=True)
                sums = sums * fade + jnp.dot(expo.astype(bf16), value, preferred_element_type=f32)
                following.append((new_peak, total, sums))
        return tuple(following)

    start = tuple(
        (
            jnp.full((rows, 1), far_below, f32),
            jnp.zeros((rows, 1), f32),
            jnp.zeros((rows, value_dim), f32),
        )
        for _ in range(2 * head_count)
    )
    state = lax.fori_loop(0, z + 1, attend, start)
    for h in range(head_count):
        _, total_a, sums_a = state[h]
        _, total_b, sums_b = state[head_count + h]
        diff = sums_a / total_a - lambdas[h] * (sums_b / total_b)
        heads[:, h * value_dim : (h + 1) * value_dim] = rms_scale(diff, head_gain[...]).astype(bf16)

    def forward(i):
        line = lax.rem(z + i, lines)
        for c in range(2):
            wz(c, line, mate // lanes, line).wait_recv()
            wx(c, line, x).start()

    early = min(2, lines - 1)
    if early > 0:
        forward(1)

    out_load.wait()
    res_load.wait()
    stream[...] = res[...].astype(f32)

    def part_copy(i):
        to = lax.rem(t + i, tp_count)
        return remote(part_out.at[to], part_in.at[t], rs_send.at[to], rs_recv.at[t], s, to)

    for i in range(1, tp_count + 1):
        to = lax.rem(t + i, tp_count)
        product = jnp.dot(
            heads[pl.ds(pl.multiple_of(to * part, 16), part), :],
            out_w[...],
            preferred_element_type=f32,
        )
        if i < tp_count:
            part_out[to] = product.astype(bf16)
            part_copy(i).start()
        else:
            stream[...] += product
    for i in range(1, tp_count):
        source = lax.rem(t + i, tp_count)
        remote(
            part_out.at[source], part_in.at[source], rs_send.at[source], rs_recv.at[source], s, source
        ).wait_recv()
        stream[...] += part_in[source].astype(f32)

    def ffn_rows(rank):
        return pl.ds(pl.multiple_of(halo + rank * part, 16), part)

    ffn[ffn_rows(t), :] = rms_scale(stream[...], mix_gain[...]).astype(bf16)

    def gather_copy(i, rank):
        to = lax.rem(t + i, tp_count)
        piece = ffn.at[ffn_rows(rank)]
        return remote(piece, piece, ag_send.at[to], ag_recv.at[rank], s, to)

    for i in range(1, tp_count):
        gather_copy(i, t).start()
    if early > 1:
        forward(2)
    for i in range(1, tp_count):
        gather_copy(i, lax.rem(t + i, tp_count)).wait_recv()

    halo_copy = remote(
        ffn.at[pl.ds(rows, halo)],
        ffn.at[pl.ds(0, halo)],
        halo_send,
        halo_recv,
        lax.rem(s + 1, sp_count),
        t,
    )

    @pl.when(s < sp_count - 1)
    def _():
        halo_copy.start()

    @pl.when(s == 0)
    def _():
        ffn[0:halo, :] = jnp.zeros((halo, width), bf16)

    @pl.when(s > 0)
    def _():
        halo_copy.wait_recv()

    acc[...] = jnp.zeros_like(acc)

    def project(first, count):
        at = pl.ds(pl.multiple_of(first, 128), count)
        for c in range(2):
            acc[c] += jnp.dot(ffn[:, at], w[c, at, :], preferred_element_type=f32)

    line_rows = lanes * w_rows
    paced = line_rows % 128 == 0

    def arrive(i):
        line = lax.rem(z + i, lines)
        for c in range(2):
            wx(c, line, 1 - x).wait_recv()
        if paced:
            project(line * line_rows, line_rows)

    if paced:
        for i in range(early + 1, lines):
            arrive(i - early - 1)
            forward(i)

        @pl.loop(max(lines - early - 1, 0), lines)
        def _(i):
            arrive(i)
    else:

        @pl.loop(early + 1, lines)
        def _(i):
            forward(i)

        @pl.loop(0, lines)
        def _(i):
            arrive(i)

        @pl.loop(0, width // 256)
        def _(i):
            project(i * 256, 256)

    @pl.loop(0, ff // 128)
    def _(i):
        at = pl.ds(pl.multiple_of(i * 128, 128), 128)
        made = []
        for c, tap in enumerate((gate_taps, up_taps)):
            total = None
            for k in range(taps):
                row = acc[c, pl.ds(halo - taps + 1 + k, rows), at].astype(bf16).astype(f32)
                term = tap[pl.ds(k, 1), at] * row
                total = term if total is None else total + term
            made.append(total)
        hidden[:, at] = (made[0] / (1 + jnp.exp(-made[0])) * made[1]).astype(bf16)

    down_load.wait()
    chunk = last_out.shape[3]

    def last_copy(i, n, rank_to, rank_from):
        return remote(
            last_out.at[rank_to, n],
            last_in.at[rank_from, n],
            last_send.at[rank_to, n],
            last_recv.at[rank_from, n],
            s,
            lax.rem(t + i, tp_count),
        )

    for n in range(width // chunk):
        product = jnp.dot(
            hidden[...], down[:, n * chunk : (n + 1) * chunk], preferred_element_type=f32
        ).astype(bf16)
        for r in range(tp_count):
            last_out[r, n] = product[r * part : (r + 1) * part]
        for i in range(1, tp_count):
            last_copy(i, n, lax.rem(t + i, tp_count), t).start()
    for n in range(width // chunk):
        at = slice(n * chunk, (n + 1) * chunk)
        total = stream[:, at] + last_out[t, n].astype(f32)
        for i in range(1, tp_count):
            source = lax.rem(t + i, tp_count)
            last_copy(i, n, source, source).wait_recv()
            total = total + last_in[source, n].astype(f32)
        out[:, at] = total.astype(bf16)

    @pl.loop(z + 1, lines)
    def _(to):
        kvz(z, to, to).wait_send()

    @pl.loop(0, z + 1)
    def _(line):
        kvx(line, x).wait_send()

    @pl.loop(1, lines)
    def _(i):
        to = lax.rem(z + i, lines)
        for c in range(2):
            wz(c, z, to, to).wait_send()

    @pl.loop(0, lines)
    def _(line):
        for c in range(2):
            wx(c, line, x).wait_send()

    for i in range(1, tp_count):
        part_copy(i).wait_send()
        gather_copy(i, t).wait_send()
        for n in range(width // chunk):
            last_copy(i, n, lax.rem(t + i, tp_count), t).wait_send()

    @pl.when(s < sp_count - 1)
    def _():
        halo_copy.wait_send()


def shards(sp_count, tp_count, *args):
    (q_a, _, _, _, vals, lambdas, head_gain, out_weight, residual, mix_gain, gate, _, _, _, down) = args
    rows = q_a.shape[0]
    width = residual.shape[1]
    w_rows, ff = gate.shape
    part = rows // tp_count
    lines = sp_count // lanes
    chunk = 512 if width % 512 == 0 else width
    args = list(args)
    args[6] = head_gain.reshape(1, -1)
    args[9] = mix_gain.reshape(1, -1)
    vmem = pl.BlockSpec(memory_space=pltpu.VMEM)
    hbm = pl.BlockSpec(memory_space=pl.ANY)
    smem = pl.BlockSpec(memory_space=pltpu.SMEM)
    dma = pltpu.SemaphoreType.DMA
    in_specs = [vmem, hbm, vmem, hbm, hbm, smem, vmem, hbm, hbm, vmem, hbm, hbm, vmem, vmem, hbm]
    return pl.pallas_call(
        functools.partial(layer, sp_count, tp_count),
        out_shape=jax.ShapeDtypeStruct((part, width), bf16),
        in_specs=in_specs,
        out_specs=vmem,
        scratch_shapes=[
            pltpu.VMEM((sp_count * rows, 2 * q_a.shape[1] + vals.shape[1]), bf16),
            pltpu.VMEM((2, sp_count * w_rows, ff), bf16),
            pltpu.VMEM(down.shape, bf16),
            pltpu.VMEM(out_weight.shape, bf16),
            pltpu.VMEM((part, width), bf16),
            pltpu.VMEM((rows, vals.shape[1]), bf16),
            pltpu.VMEM((tp_count, part, width), bf16),
            pltpu.VMEM((tp_count, part, width), bf16),
            pltpu.VMEM((part, width), f32),
            pltpu.VMEM((halo + rows, width), bf16),
            pltpu.VMEM((2, halo + rows, ff), f32),
            pltpu.VMEM((rows, ff), bf16),
            pltpu.VMEM((tp_count, width // chunk, part, chunk), bf16),
            pltpu.VMEM((tp_count, width // chunk, part, chunk), bf16),
            dma((8,)),
            dma((lines,)),
            dma((lines,)),
            dma((lines,)),
            dma((lines,)),
            dma((2, lines)),
            dma((2, lines)),
            dma((2, lines)),
            dma((2, lines)),
            dma((tp_count,)),
            dma((tp_count,)),
            dma((tp_count,)),
            dma((tp_count,)),
            dma(()),
            dma(()),
            dma((tp_count, width // chunk)),
            dma((tp_count, width // chunk)),
        ],
        compiler_params=pltpu.CompilerParams(
            collective_id=0, has_side_effects=True, vmem_limit_bytes=60 * 1024 * 1024
        ),
    )(*args)


def solution(mesh):
    in_specs = (
        P("sp", "tp"),
        P("sp", "tp"),
        P("sp", "tp"),
        P("sp", "tp"),
        P("sp", "tp"),
        P("tp"),
        P(),
        P("tp", None),
        P("sp", None),
        P(),
        P("sp", "tp"),
        P("sp", "tp"),
        P(None, "tp"),
        P(None, "tp"),
        P("tp", None),
    )
    body = functools.partial(shards, mesh.shape["sp"], mesh.shape["tp"])
    return jax.shard_map(
        body, mesh=mesh, in_specs=in_specs, out_specs=P(("sp", "tp"), None), check_vma=False
    )
```

```python
import functools

import jax
import jax.numpy as jnp
from jax import lax
from jax.experimental import pallas as pl
from jax.experimental.pallas import tpu as pltpu
from jax.sharding import PartitionSpec as P

norm_eps = 1e-06
far_below = -1e30
halo = 16
lanes = 2
team = 2
f32 = jnp.float32
bf16 = jnp.bfloat16


def rms_scale(field, gain):
    return field * lax.rsqrt(jnp.mean(field * field, axis=-1, keepdims=True) + norm_eps) * gain


def layer(
    sp_count,
    tp_count,
    q_a,
    k_a,
    q_b,
    k_b,
    vals,
    lambdas,
    head_gain,
    out_weight,
    residual,
    mix_gain,
    gate_weight,
    up_weight,
    gate_taps,
    up_taps,
    down_weight,
    out,
    kv,
    w_own,
    w,
    down,
    out_w,
    res,
    heads,
    part_out,
    part_in,
    stream,
    ffn,
    acc,
    hidden,
    last_out,
    last_in,
    local,
    kvz_send,
    kvz_recv,
    kvx_send,
    kvx_recv,
    wz_send,
    wz_recv,
    wx_send,
    wx_recv,
    rs_send,
    rs_recv,
    ag_send,
    ag_recv,
    halo_send,
    halo_recv,
    last_send,
    last_recv,
):
    s = lax.axis_index("sp")
    t = lax.axis_index("tp")
    x = lax.rem(s, lanes)
    z = s // lanes
    lines = sp_count // lanes
    mate = z * lanes + (1 - x)
    rows = q_a.shape[0]
    key_width = q_a.shape[1]
    value_width = vals.shape[1]
    head_count = lambdas.shape[0]
    head_dim = key_width // head_count
    value_dim = value_width // head_count
    part = rows // tp_count
    width = out.shape[1]
    w_rows = gate_weight.shape[0]
    ff = gate_weight.shape[1]
    taps = gate_taps.shape[0]
    piece = w.shape[2]
    shift = ff - piece
    g = lax.rem(z, team)
    partner = (z + 1 - 2 * g) * lanes + x
    slot_rows = halo + rows

    def columns(line):
        return pl.multiple_of(lax.rem(line, team) * shift, 128)


    def remote(src, dst, send, recv, sp, tp):
        return pltpu.make_async_remote_copy(
            src_ref=src,
            dst_ref=dst,
            send_sem=send,
            recv_sem=recv,
            device_id=(sp, tp),
            device_id_type=pl.DeviceIdType.MESH,
        )

    def kv_block(block):
        return kv.at[pl.ds(pl.multiple_of(block * rows, 16), rows)]

    def w_block(c, block):
        return w.at[c, pl.ds(pl.multiple_of(block * w_rows, 16), w_rows)]

    own = pl.ds(pl.multiple_of(s * rows, 16), rows)
    kv_loads = (
        pltpu.make_async_copy(k_a, kv.at[own, pl.ds(0, key_width)], local.at[0]),
        pltpu.make_async_copy(k_b, kv.at[own, pl.ds(key_width, key_width)], local.at[1]),
        pltpu.make_async_copy(vals, kv.at[own, pl.ds(2 * key_width, value_width)], local.at[2]),
    )
    w_loads = (
        pltpu.make_async_copy(gate_weight, w_own.at[0], local.at[3]),
        pltpu.make_async_copy(up_weight, w_own.at[1], local.at[4]),
        pltpu.make_async_copy(gate_weight.at[:, pl.ds(columns(z), piece)], w_block(0, s), local.at[8]),
        pltpu.make_async_copy(up_weight.at[:, pl.ds(columns(z), piece)], w_block(1, s), local.at[9]),
    )
    out_load = pltpu.make_async_copy(out_weight, out_w, local.at[5])
    res_load = pltpu.make_async_copy(
        residual.at[pl.ds(pl.multiple_of(t * part, 16), part)], res, local.at[6]
    )
    down_load = pltpu.make_async_copy(down_weight.at[pl.ds(columns(z), piece)], down, local.at[7])
    for load in kv_loads + w_loads + (out_load, res_load, down_load):
        load.start()

    barrier = pltpu.get_barrier_semaphore()

    @pl.loop(1, sp_count)
    def _(i):
        pl.semaphore_signal(
            barrier,
            inc=1,
            device_id=(lax.rem(s + i, sp_count), t),
            device_id_type=pl.DeviceIdType.MESH,
        )

    @pl.loop(1, tp_count)
    def _(i):
        pl.semaphore_signal(
            barrier,
            inc=1,
            device_id=(s, lax.rem(t + i, tp_count)),
            device_id_type=pl.DeviceIdType.MESH,
        )

    for i in range(1, tp_count):
        pl.semaphore_signal(
            barrier,
            inc=1,
            device_id=(partner, lax.rem(t + i, tp_count)),
            device_id_type=pl.DeviceIdType.MESH,
        )

    pl.semaphore_wait(barrier, sp_count + 2 * tp_count - 3)

    def kvz(line, to, index):
        block = kv_block(line * lanes + x)
        return remote(block, block, kvz_send.at[index], kvz_recv.at[line], to * lanes + x, t)

    def kvx(line, lane):
        block = kv_block(line * lanes + lane)
        return remote(block, block, kvx_send.at[line], kvx_recv.at[line], mate, t)

    def wz(c, line, to, index):
        block = w_block(c, line * lanes + x)
        source = w_own.at[c, :, pl.ds(columns(to), piece)]
        return remote(source, block, wz_send.at[c, index], wz_recv.at[c, line], to * lanes + x, t)

    def wx(c, line, lane):
        block = w_block(c, line * lanes + lane)
        return remote(block, block, wx_send.at[c, line], wx_recv.at[c, line], mate, t)

    for load in kv_loads:
        load.wait()

    @pl.loop(z + 1, lines)
    def _(to):
        kvz(z, to, to).start()

    kvx(z, x).start()
    for load in w_loads:
        load.wait()

    @pl.loop(1, lines)
    def _(i):
        to = lax.rem(z + lines - i, lines)
        for c in range(2):
            wz(c, z, to, to).start()

    @pl.loop(0, z)
    def _(i):
        line = z - 1 - i
        kvz(line, mate // lanes, line).wait_recv()
        kvx(line, x).start()

    for c in range(2):
        wx(c, z, x).start()

    scale = head_dim**-0.5
    column = lax.broadcasted_iota(jnp.int32, (rows, key_width), 1) // head_dim
    queries = [
        jnp.where(column == h, q[...], jnp.zeros((), bf16))
        for q in (q_a, q_b)
        for h in range(head_count)
    ]
    span = lanes * rows
    query_pos = s * rows + lax.broadcasted_iota(jnp.int32, (rows, span), 0)
    key_step = lax.broadcasted_iota(jnp.int32, (rows, span), 1)

    def attend(i, state):
        line = z - i
        kvx(line, 1 - x).wait_recv()
        keys_at = pl.ds(pl.multiple_of(line * span, 16), span)
        visible = line * span + key_step <= query_pos
        following = []
        for m in range(2):
            keys = kv[keys_at, pl.ds(m * key_width, key_width)]
            for h in range(head_count):
                peak, total, sums = state[m * head_count + h]
                value = kv[keys_at, pl.ds(2 * key_width + h * value_dim, value_dim)]
                scores = (
                    lax.dot_general(
                        queries[m * head_count + h],
                        keys,
                        (((1,), (1,)), ((), ())),
                        preferred_element_type=f32,
                    )
                    * scale
                )
                scores = jnp.where(visible, scores, far_below)
                new_peak = jnp.maximum(peak, jnp.max(scores, axis=-1, keepdims=True))
                fade = jnp.exp(peak - new_peak)
                expo = jnp.exp(scores - new_peak)
                total = total * fade + jnp.sum(expo, axis=-1, keepdims=True)
                sums = sums * fade + jnp.dot(expo.astype(bf16), value, preferred_element_type=f32)
                following.append((new_peak, total, sums))
        return tuple(following)

    start = tuple(
        (
            jnp.full((rows, 1), far_below, f32),
            jnp.zeros((rows, 1), f32),
            jnp.zeros((rows, value_dim), f32),
        )
        for _ in range(2 * head_count)
    )
    state = lax.fori_loop(0, z + 1, attend, start)
    for h in range(head_count):
        _, total_a, sums_a = state[h]
        _, total_b, sums_b = state[head_count + h]
        diff = sums_a / total_a - lambdas[h] * (sums_b / total_b)
        heads[:, h * value_dim : (h + 1) * value_dim] = rms_scale(diff, head_gain[...]).astype(bf16)

    def forward(i):
        line = lax.rem(z + i, lines)
        for c in range(2):
            wz(c, line, mate // lanes, line).wait_recv()
            wx(c, line, x).start()

    early = min(2, lines - 1)
    if early > 0:
        forward(1)

    out_load.wait()
    res_load.wait()
    stream[...] = res[...].astype(f32)

    def part_copy(i):
        to = lax.rem(t + i, tp_count)
        return remote(part_out.at[to], part_in.at[t], rs_send.at[to], rs_recv.at[t], s, to)

    for i in range(1, tp_count + 1):
        to = lax.rem(t + i, tp_count)
        product = jnp.dot(
            heads[pl.ds(pl.multiple_of(to * part, 16), part), :],
            out_w[...],
            preferred_element_type=f32,
        )
        if i < tp_count:
            part_out[to] = product.astype(bf16)
            part_copy(i).start()
        else:
            stream[...] += product
    for i in range(1, tp_count):
        source = lax.rem(t + i, tp_count)
        remote(
            part_out.at[source], part_in.at[source], rs_send.at[source], rs_recv.at[source], s, source
        ).wait_recv()
        stream[...] += part_in[source].astype(f32)

    def ffn_rows(slot, rank):
        return pl.ds(pl.multiple_of(slot * slot_rows + halo + rank * part, 16), part)

    ffn[ffn_rows(g, t), :] = rms_scale(stream[...], mix_gain[...]).astype(bf16)

    def team_copy(slot):
        rows_here = ffn.at[ffn_rows(slot, t)]
        return remote(rows_here, rows_here, ag_send.at[slot, t], ag_recv.at[slot, t], partner, t)

    def gather_copy(i, slot, rank):
        to = lax.rem(t + i, tp_count)
        rows_here = ffn.at[ffn_rows(slot, rank)]
        return remote(rows_here, rows_here, ag_send.at[slot, to], ag_recv.at[slot, rank], s, to)

    team_copy(g).start()
    for i in range(1, tp_count):
        gather_copy(i, g, t).start()
    if early > 1:
        forward(2)
    for i in range(1, tp_count):
        gather_copy(i, g, lax.rem(t + i, tp_count)).wait_recv()

    after = lax.rem(s + 1, sp_count)
    after_line = after // lanes
    after_slot = lax.rem(after_line, team)
    after_other = (after_line + 1 - 2 * after_slot) * lanes + lax.rem(after, lanes)

    def halo_copy(which, target, slot):
        return remote(
            ffn.at[pl.ds(pl.multiple_of(g * slot_rows + rows, 16), halo)],
            ffn.at[pl.ds(pl.multiple_of(slot * slot_rows, 16), halo)],
            halo_send.at[which],
            halo_recv.at[slot],
            target,
            t,
        )

    @pl.when(s < sp_count - 1)
    def _():
        halo_copy(0, after, after_slot).start()

        halo_copy(1, after_other, after_slot).start()

    team_copy(1 - g).wait_recv()
    for i in range(1, tp_count):
        gather_copy(i, 1 - g, t).start()

    for slot in range(team):
        block = (z - g + slot) * lanes + x

        @pl.when(block == 0)
        def _():
            ffn[slot * slot_rows : slot * slot_rows + halo, :] = jnp.zeros((halo, width), bf16)

        @pl.when(block > 0)
        def _():
            halo_copy(0, mate, slot).wait_recv()

    for i in range(1, tp_count):
        gather_copy(i, 1 - g, lax.rem(t + i, tp_count)).wait_recv()

    acc[...] = jnp.zeros_like(acc)

    def project(first, count):
        at = pl.ds(pl.multiple_of(first, 128), count)
        for c in range(2):
            acc[c] += jnp.dot(ffn[:, at], w[c, at, :], preferred_element_type=f32)

    line_rows = lanes * w_rows
    paced = line_rows % 128 == 0

    def arrive(i):
        line = lax.rem(z + i, lines)
        for c in range(2):
            wx(c, line, 1 - x).wait_recv()
        if paced:
            project(line * line_rows, line_rows)

    if paced:
        for i in range(early + 1, lines):
            arrive(i - early - 1)
            forward(i)

        @pl.loop(max(lines - early - 1, 0), lines)
        def _(i):
            arrive(i)
    else:

        @pl.loop(early + 1, lines)
        def _(i):
            forward(i)

        @pl.loop(0, lines)
        def _(i):
            arrive(i)

        @pl.loop(0, width // 256)
        def _(i):
            project(i * 256, 256)

    @pl.loop(0, piece // 128)
    def _(i):
        at = pl.ds(pl.multiple_of(i * 128, 128), 128)
        tap_at = pl.ds(pl.multiple_of(columns(z) + i * 128, 128), 128)
        fresh = i * 128 >= g * (piece - shift)
        for slot in range(team):
            made = []
            for c, tap in enumerate((gate_taps, up_taps)):
                total = None
                for k in range(taps):
                    first = slot * slot_rows + halo - taps + 1 + k
                    row = acc[c, pl.ds(first, rows), at].astype(bf16).astype(f32)
                    term = tap[pl.ds(k, 1), tap_at] * row
                    total = term if total is None else total + term
                made.append(total)
            value = made[0] / (1 + jnp.exp(-made[0])) * made[1]
            hidden[slot * rows : (slot + 1) * rows, at] = jnp.where(fresh, value, 0.0).astype(bf16)

    down_load.wait()
    chunk = last_out.shape[3]

    def last_copy(n, far, rank, source, source_far):
        return remote(
            last_out.at[far * tp_count + rank, n],
            last_in.at[source_far * tp_count + source, n],
            last_send.at[far * tp_count + rank, n],
            last_recv.at[source_far * tp_count + source, n],
            partner if far else s,
            rank,
        )

    for n in range(width // chunk):
        for far in (1, 0):
            slot = 1 - g if far else g
            product = jnp.dot(
                hidden[pl.ds(pl.multiple_of(slot * rows, 16), rows), :],
                down[:, n * chunk : (n + 1) * chunk],
                preferred_element_type=f32,
            ).astype(bf16)
            for r in range(tp_count):
                last_out[far * tp_count + r, n] = product[r * part : (r + 1) * part]
            for i in range(1 - far, tp_count):
                last_copy(n, far, lax.rem(t + i, tp_count), t, far).start()
    for n in range(width // chunk):
        at = slice(n * chunk, (n + 1) * chunk)
        total = stream[:, at] + last_out[t, n].astype(f32)
        for far in (0, 1):
            for i in range(1 - far, tp_count):
                source = lax.rem(t + i, tp_count)
                last_copy(n, far, source, source, far).wait_recv()
                total = total + last_in[far * tp_count + source, n].astype(f32)
        out[:, at] = total.astype(bf16)

    @pl.loop(z + 1, lines)
    def _(to):
        kvz(z, to, to).wait_send()

    @pl.loop(0, z + 1)
    def _(line):
        kvx(line, x).wait_send()

    @pl.loop(1, lines)
    def _(i):
        to = lax.rem(z + i, lines)
        for c in range(2):
            wz(c, z, to, to).wait_send()

    @pl.loop(0, lines)
    def _(line):
        for c in range(2):
            wx(c, line, x).wait_send()

    team_copy(g).wait_send()
    for i in range(1, tp_count):
        part_copy(i).wait_send()
        for slot in range(team):
            gather_copy(i, slot, t).wait_send()
    for n in range(width // chunk):
        for far in (0, 1):
            for i in range(1 - far, tp_count):
                last_copy(n, far, lax.rem(t + i, tp_count), t, far).wait_send()

    @pl.when(s < sp_count - 1)
    def _():
        halo_copy(0, after, after_slot).wait_send()

        halo_copy(1, after_other, after_slot).wait_send()


def shards(sp_count, tp_count, *args):
    (q_a, _, _, _, vals, lambdas, head_gain, out_weight, residual, mix_gain, gate, _, _, _, down) = args
    rows = q_a.shape[0]
    width = residual.shape[1]
    w_rows, ff = gate.shape
    part = rows // tp_count
    lines = sp_count // lanes
    chunk = 512 if width % 512 == 0 else width
    piece = -(-ff // (team * 128)) * 128
    args = list(args)
    args[6] = head_gain.reshape(1, -1)
    args[9] = mix_gain.reshape(1, -1)
    vmem = pl.BlockSpec(memory_space=pltpu.VMEM)
    hbm = pl.BlockSpec(memory_space=pl.ANY)
    smem = pl.BlockSpec(memory_space=pltpu.SMEM)
    dma = pltpu.SemaphoreType.DMA
    in_specs = [vmem, hbm, vmem, hbm, hbm, smem, vmem, hbm, hbm, vmem, hbm, hbm, vmem, vmem, hbm]
    return pl.pallas_call(
        functools.partial(layer, sp_count, tp_count),
        out_shape=jax.ShapeDtypeStruct((part, width), bf16),
        in_specs=in_specs,
        out_specs=vmem,
        scratch_shapes=[
            pltpu.VMEM((sp_count * rows, 2 * q_a.shape[1] + vals.shape[1]), bf16),
            pltpu.VMEM((2, w_rows, ff), bf16),
            pltpu.VMEM((2, sp_count * w_rows, piece), bf16),
            pltpu.VMEM((piece, width), bf16),
            pltpu.VMEM(out_weight.shape, bf16),
            pltpu.VMEM((part, width), bf16),
            pltpu.VMEM((rows, vals.shape[1]), bf16),
            pltpu.VMEM((tp_count, part, width), bf16),
            pltpu.VMEM((tp_count, part, width), bf16),
            pltpu.VMEM((part, width), f32),
            pltpu.VMEM((team * (halo + rows), width), bf16),
            pltpu.VMEM((2, team * (halo + rows), piece), f32),
            pltpu.VMEM((team * rows, piece), bf16),
            pltpu.VMEM((team * tp_count, width // chunk, part, chunk), bf16),
            pltpu.VMEM((team * tp_count, width // chunk, part, chunk), bf16),
            dma((10,)),
            dma((lines,)),
            dma((lines,)),
            dma((lines,)),
            dma((lines,)),
            dma((2, lines)),
            dma((2, lines)),
            dma((2, lines)),
            dma((2, lines)),
            dma((tp_count,)),
            dma((tp_count,)),
            dma((team, tp_count)),
            dma((team, tp_count)),
            dma((2,)),
            dma((team,)),
            dma((team * tp_count, width // chunk)),
            dma((team * tp_count, width // chunk)),
        ],
        compiler_params=pltpu.CompilerParams(
            collective_id=0, has_side_effects=True, vmem_limit_bytes=60 * 1024 * 1024
        ),
    )(*args)


def solution(mesh):
    in_specs = (
        P("sp", "tp"),
        P("sp", "tp"),
        P("sp", "tp"),
        P("sp", "tp"),
        P("sp", "tp"),
        P("tp"),
        P(),
        P("tp", None),
        P("sp", None),
        P(),
        P("sp", "tp"),
        P("sp", "tp"),
        P(None, "tp"),
        P(None, "tp"),
        P("tp", None),
    )
    body = functools.partial(shards, mesh.shape["sp"], mesh.shape["tp"])
    return jax.shard_map(
        body, mesh=mesh, in_specs=in_specs, out_specs=P(("sp", "tp"), None), check_vma=False
    )
```

```python
import functools

import jax
import jax.numpy as jnp
from jax import lax
from jax.experimental import pallas as pl
from jax.experimental.pallas import tpu as pltpu
from jax.sharding import PartitionSpec as P

norm_eps = 1e-06
far_below = -1e30
halo = 16
lanes = 2
team = 2
f32 = jnp.float32
bf16 = jnp.bfloat16


def rms_scale(field, gain):
    return field * lax.rsqrt(jnp.mean(field * field, axis=-1, keepdims=True) + norm_eps) * gain


def layer(
    sp_count,
    tp_count,
    q_a,
    k_a,
    q_b,
    k_b,
    vals,
    lambdas,
    head_gain,
    out_weight,
    residual,
    mix_gain,
    gate_weight,
    up_weight,
    gate_taps,
    up_taps,
    down_weight,
    out,
    kv,
    w_own,
    w,
    down,
    out_w,
    res,
    heads,
    part_out,
    part_in,
    stream,
    ffn,
    acc,
    hidden,
    pair_out,
    pair_in,
    last_out,
    last_in,
    local,
    kvz_send,
    kvz_recv,
    kvx_send,
    kvx_recv,
    wz_send,
    wz_recv,
    wx_send,
    wx_recv,
    rs_send,
    rs_recv,
    ag_send,
    ag_recv,
    halo_send,
    halo_recv,
    pair_send,
    pair_recv,
    last_send,
    last_recv,
):
    s = lax.axis_index("sp")
    t = lax.axis_index("tp")
    x = lax.rem(s, lanes)
    z = s // lanes
    lines = sp_count // lanes
    mate = z * lanes + (1 - x)
    rows = q_a.shape[0]
    key_width = q_a.shape[1]
    value_width = vals.shape[1]
    head_count = lambdas.shape[0]
    head_dim = key_width // head_count
    value_dim = value_width // head_count
    part = rows // tp_count
    width = out.shape[1]
    w_rows = gate_weight.shape[0]
    ff = gate_weight.shape[1]
    taps = gate_taps.shape[0]
    piece = w.shape[2]
    shift = ff - piece
    g = lax.rem(z, team)
    partner = (z + 1 - 2 * g) * lanes + x
    slot_rows = halo + rows

    def columns(line):
        return pl.multiple_of(lax.rem(line, team) * shift, 128)


    def remote(src, dst, send, recv, sp, tp):
        return pltpu.make_async_remote_copy(
            src_ref=src,
            dst_ref=dst,
            send_sem=send,
            recv_sem=recv,
            device_id=(sp, tp),
            device_id_type=pl.DeviceIdType.MESH,
        )

    def kv_block(block):
        return kv.at[pl.ds(pl.multiple_of(block * rows, 16), rows)]

    def w_block(c, block):
        return w.at[c, pl.ds(pl.multiple_of(block * w_rows, 16), w_rows)]

    own = pl.ds(pl.multiple_of(s * rows, 16), rows)
    kv_loads = (
        pltpu.make_async_copy(k_a, kv.at[own, pl.ds(0, key_width)], local.at[0]),
        pltpu.make_async_copy(k_b, kv.at[own, pl.ds(key_width, key_width)], local.at[1]),
        pltpu.make_async_copy(vals, kv.at[own, pl.ds(2 * key_width, value_width)], local.at[2]),
    )
    w_loads = (
        pltpu.make_async_copy(gate_weight, w_own.at[0], local.at[3]),
        pltpu.make_async_copy(up_weight, w_own.at[1], local.at[4]),
        pltpu.make_async_copy(gate_weight.at[:, pl.ds(columns(z), piece)], w_block(0, s), local.at[8]),
        pltpu.make_async_copy(up_weight.at[:, pl.ds(columns(z), piece)], w_block(1, s), local.at[9]),
    )
    out_load = pltpu.make_async_copy(out_weight, out_w, local.at[5])
    res_load = pltpu.make_async_copy(
        residual.at[pl.ds(pl.multiple_of(t * part, 16), part)], res, local.at[6]
    )
    down_load = pltpu.make_async_copy(down_weight.at[pl.ds(columns(z), piece)], down, local.at[7])
    for load in kv_loads + w_loads + (out_load, res_load, down_load):
        load.start()

    barrier = pltpu.get_barrier_semaphore()

    @pl.loop(1, sp_count)
    def _(i):
        pl.semaphore_signal(
            barrier,
            inc=1,
            device_id=(lax.rem(s + i, sp_count), t),
            device_id_type=pl.DeviceIdType.MESH,
        )

    @pl.loop(1, tp_count)
    def _(i):
        pl.semaphore_signal(
            barrier,
            inc=1,
            device_id=(s, lax.rem(t + i, tp_count)),
            device_id_type=pl.DeviceIdType.MESH,
        )

    for i in range(1, tp_count):
        pl.semaphore_signal(
            barrier,
            inc=1,
            device_id=(partner, lax.rem(t + i, tp_count)),
            device_id_type=pl.DeviceIdType.MESH,
        )

    pl.semaphore_wait(barrier, sp_count + 2 * tp_count - 3)

    def kvz(line, to, index):
        block = kv_block(line * lanes + x)
        return remote(block, block, kvz_send.at[index], kvz_recv.at[line], to * lanes + x, t)

    def kvx(line, lane):
        block = kv_block(line * lanes + lane)
        return remote(block, block, kvx_send.at[line], kvx_recv.at[line], mate, t)

    def wz(c, line, to, index):
        block = w_block(c, line * lanes + x)
        source = w_own.at[c, :, pl.ds(columns(to), piece)]
        return remote(source, block, wz_send.at[c, index], wz_recv.at[c, line], to * lanes + x, t)

    def wx(c, line, lane):
        block = w_block(c, line * lanes + lane)
        return remote(block, block, wx_send.at[c, line], wx_recv.at[c, line], mate, t)

    for load in kv_loads:
        load.wait()

    @pl.loop(z + 1, lines)
    def _(to):
        kvz(z, to, to).start()

    kvx(z, x).start()
    for load in w_loads:
        load.wait()

    def send_weights(i):
        to = lax.rem(z + lines - i, lines)
        for c in range(2):
            wz(c, z, to, to).start()

    @pl.loop(1, lines - 1)
    def _(i):
        send_weights(i)

    @pl.loop(0, z)
    def _(i):
        line = z - 1 - i
        kvz(line, mate // lanes, line).wait_recv()
        kvx(line, x).start()

    for c in range(2):
        wx(c, z, x).start()

    scale = head_dim**-0.5
    column = lax.broadcasted_iota(jnp.int32, (rows, key_width), 1) // head_dim
    queries = [
        jnp.where(column == h, q[...], jnp.zeros((), bf16))
        for q in (q_a, q_b)
        for h in range(head_count)
    ]
    span = lanes * rows
    query_pos = s * rows + lax.broadcasted_iota(jnp.int32, (rows, span), 0)
    key_step = lax.broadcasted_iota(jnp.int32, (rows, span), 1)

    def attend(i, state):
        line = z - i
        kvx(line, 1 - x).wait_recv()
        keys_at = pl.ds(pl.multiple_of(line * span, 16), span)
        visible = line * span + key_step <= query_pos
        following = []
        for m in range(2):
            keys = kv[keys_at, pl.ds(m * key_width, key_width)]
            for h in range(head_count):
                peak, total, sums = state[m * head_count + h]
                value = kv[keys_at, pl.ds(2 * key_width + h * value_dim, value_dim)]
                scores = (
                    lax.dot_general(
                        queries[m * head_count + h],
                        keys,
                        (((1,), (1,)), ((), ())),
                        preferred_element_type=f32,
                    )
                    * scale
                )
                scores = jnp.where(visible, scores, far_below)
                new_peak = jnp.maximum(peak, jnp.max(scores, axis=-1, keepdims=True))
                fade = jnp.exp(peak - new_peak)
                expo = jnp.exp(scores - new_peak)
                total = total * fade + jnp.sum(expo, axis=-1, keepdims=True)
                sums = sums * fade + jnp.dot(expo.astype(bf16), value, preferred_element_type=f32)
                following.append((new_peak, total, sums))
        return tuple(following)

    start = tuple(
        (
            jnp.full((rows, 1), far_below, f32),
            jnp.zeros((rows, 1), f32),
            jnp.zeros((rows, value_dim), f32),
        )
        for _ in range(2 * head_count)
    )
    state = lax.fori_loop(0, z + 1, attend, start)
    for h in range(head_count):
        _, total_a, sums_a = state[h]
        _, total_b, sums_b = state[head_count + h]
        diff = sums_a / total_a - lambdas[h] * (sums_b / total_b)
        heads[:, h * value_dim : (h + 1) * value_dim] = rms_scale(diff, head_gain[...]).astype(bf16)

    def forward(i):
        line = lax.rem(z + i, lines)
        for c in range(2):
            wz(c, line, mate // lanes, line).wait_recv()
            wx(c, line, x).start()

    early = min(3, lines - 1)
    if early > 0:
        forward(1)

    out_load.wait()
    res_load.wait()
    stream[...] = res[...].astype(f32)

    def part_copy(i):
        to = lax.rem(t + i, tp_count)
        return remote(part_out.at[to], part_in.at[t], rs_send.at[to], rs_recv.at[t], s, to)

    for i in range(1, tp_count + 1):
        to = lax.rem(t + i, tp_count)
        product = jnp.dot(
            heads[pl.ds(pl.multiple_of(to * part, 16), part), :],
            out_w[...],
            preferred_element_type=f32,
        )
        if i < tp_count:
            part_out[to] = product.astype(bf16)
            part_copy(i).start()
        else:
            stream[...] += product
    for i in range(1, tp_count):
        source = lax.rem(t + i, tp_count)
        remote(
            part_out.at[source], part_in.at[source], rs_send.at[source], rs_recv.at[source], s, source
        ).wait_recv()
        stream[...] += part_in[source].astype(f32)

    def ffn_rows(slot, rank):
        return pl.ds(pl.multiple_of(slot * slot_rows + halo + rank * part, 16), part)

    ffn[ffn_rows(g, t), :] = rms_scale(stream[...], mix_gain[...]).astype(bf16)

    def team_copy(slot):
        rows_here = ffn.at[ffn_rows(slot, t)]
        return remote(rows_here, rows_here, ag_send.at[slot, t], ag_recv.at[slot, t], partner, t)

    def gather_copy(i, slot, rank):
        to = lax.rem(t + i, tp_count)
        rows_here = ffn.at[ffn_rows(slot, rank)]
        return remote(rows_here, rows_here, ag_send.at[slot, to], ag_recv.at[slot, rank], s, to)

    team_copy(g).start()
    send_weights(lines - 1)
    for i in range(1, tp_count):
        gather_copy(i, g, t).start()
    if early > 1:
        forward(2)
    for i in range(1, tp_count):
        gather_copy(i, g, lax.rem(t + i, tp_count)).wait_recv()

    after = lax.rem(s + 1, sp_count)
    after_line = after // lanes
    after_slot = lax.rem(after_line, team)
    after_other = (after_line + 1 - 2 * after_slot) * lanes + lax.rem(after, lanes)

    def halo_copy(which, target, slot):
        return remote(
            ffn.at[pl.ds(pl.multiple_of(g * slot_rows + rows, 16), halo)],
            ffn.at[pl.ds(pl.multiple_of(slot * slot_rows, 16), halo)],
            halo_send.at[which],
            halo_recv.at[slot],
            target,
            t,
        )

    @pl.when(s < sp_count - 1)
    def _():
        halo_copy(0, after, after_slot).start()

        halo_copy(1, after_other, after_slot).start()

    team_copy(1 - g).wait_recv()
    for i in range(1, tp_count):
        gather_copy(i, 1 - g, t).start()
    if early > 2:
        forward(3)

    for slot in range(team):
        block = (z - g + slot) * lanes + x

        @pl.when(block == 0)
        def _():
            ffn[slot * slot_rows : slot * slot_rows + halo, :] = jnp.zeros((halo, width), bf16)

        @pl.when(block > 0)
        def _():
            halo_copy(0, mate, slot).wait_recv()

    for i in range(1, tp_count):
        gather_copy(i, 1 - g, lax.rem(t + i, tp_count)).wait_recv()

    acc[...] = jnp.zeros_like(acc)

    def project(first, count):
        at = pl.ds(pl.multiple_of(first, 128), count)
        for c in range(2):
            acc[c] += jnp.dot(ffn[:, at], w[c, at, :], preferred_element_type=f32)

    line_rows = lanes * w_rows
    paced = line_rows % 128 == 0

    def arrive(i):
        line = lax.rem(z + i, lines)
        for c in range(2):
            wx(c, line, 1 - x).wait_recv()
        if paced:
            project(line * line_rows, line_rows)

    if paced:
        for i in range(early + 1, lines):
            arrive(i - early - 1)
            forward(i)

        @pl.loop(max(lines - early - 1, 0), lines)
        def _(i):
            arrive(i)
    else:

        @pl.loop(early + 1, lines)
        def _(i):
            forward(i)

        @pl.loop(0, lines)
        def _(i):
            arrive(i)

        @pl.loop(0, width // 256)
        def _(i):
            project(i * 256, 256)

    @pl.loop(0, piece // 128)
    def _(i):
        at = pl.ds(pl.multiple_of(i * 128, 128), 128)
        tap_at = pl.ds(pl.multiple_of(columns(z) + i * 128, 128), 128)
        fresh = i * 128 >= g * (piece - shift)
        for slot in range(team):
            made = []
            for c, tap in enumerate((gate_taps, up_taps)):
                total = None
                for k in range(taps):
                    first = slot * slot_rows + halo - taps + 1 + k
                    row = acc[c, pl.ds(first, rows), at].astype(bf16).astype(f32)
                    term = tap[pl.ds(k, 1), tap_at] * row
                    total = term if total is None else total + term
                made.append(total)
            value = made[0] / (1 + jnp.exp(-made[0])) * made[1]
            hidden[slot * rows : (slot + 1) * rows, at] = jnp.where(fresh, value, 0.0).astype(bf16)

    down_load.wait()
    chunk = last_out.shape[2]
    chunks = width // chunk
    pairs = tp_count // 2
    c_own = lax.rem(t, 2)
    k_own = t // 2

    def pair_rows(far, k):
        return pl.ds(pl.multiple_of((far * pairs + k) * part, 16), part)

    def pair_copy(n):
        return remote(
            pair_out.at[n, 1 - c_own],
            pair_in.at[n],
            pair_send.at[n],
            pair_recv.at[n],
            s,
            t + 1 - 2 * c_own,
        )

    def last_copy(n, far, k, source):
        return remote(
            last_out.at[n, pair_rows(far, k)],
            last_in.at[n, pair_rows(far, source)],
            last_send.at[n, far * pairs + k],
            last_recv.at[n, far * pairs + source],
            partner if far else s,
            2 * k + c_own,
        )

    for n in range(chunks + 1):
        if n < chunks:
            for far in (1, 0):
                slot = 1 - g if far else g
                product = jnp.dot(
                    hidden[pl.ds(pl.multiple_of(slot * rows, 16), rows), :],
                    down[:, n * chunk : (n + 1) * chunk],
                    preferred_element_type=f32,
                ).astype(bf16)
                for r in range(tp_count):
                    first = (far * pairs + r // 2) * part
                    pair_out[n, r % 2, first : first + part] = product[r * part : (r + 1) * part]
            pair_copy(n).start()
        if n > 0:
            pair_copy(n - 1).wait_recv()
            both = pair_out[n - 1, c_own].astype(f32) + pair_in[n - 1].astype(f32)
            last_out[n - 1] = both.astype(bf16)
            for far in (1, 0):
                for i in range(1 - far, pairs):
                    last_copy(n - 1, far, lax.rem(k_own + i, pairs), k_own).start()
    for n in range(chunks):
        at = slice(n * chunk, (n + 1) * chunk)
        total = stream[:, at] + last_out[n, pair_rows(0, k_own), :].astype(f32)
        for far in (0, 1):
            for i in range(1 - far, pairs):
                source = lax.rem(k_own + i, pairs)
                last_copy(n, far, source, source).wait_recv()
                total = total + last_in[n, pair_rows(far, source), :].astype(f32)
        out[:, at] = total.astype(bf16)

    @pl.loop(z + 1, lines)
    def _(to):
        kvz(z, to, to).wait_send()

    @pl.loop(0, z + 1)
    def _(line):
        kvx(line, x).wait_send()

    @pl.loop(1, lines)
    def _(i):
        to = lax.rem(z + i, lines)
        for c in range(2):
            wz(c, z, to, to).wait_send()

    @pl.loop(0, lines)
    def _(line):
        for c in range(2):
            wx(c, line, x).wait_send()

    team_copy(g).wait_send()
    for i in range(1, tp_count):
        part_copy(i).wait_send()
        for slot in range(team):
            gather_copy(i, slot, t).wait_send()
    for n in range(chunks):
        pair_copy(n).wait_send()
        for far in (0, 1):
            for i in range(1 - far, pairs):
                last_copy(n, far, lax.rem(k_own + i, pairs), k_own).wait_send()

    @pl.when(s < sp_count - 1)
    def _():
        halo_copy(0, after, after_slot).wait_send()

        halo_copy(1, after_other, after_slot).wait_send()


def shards(sp_count, tp_count, *args):
    (q_a, _, _, _, vals, lambdas, head_gain, out_weight, residual, mix_gain, gate, _, _, _, down) = args
    rows = q_a.shape[0]
    width = residual.shape[1]
    w_rows, ff = gate.shape
    part = rows // tp_count
    lines = sp_count // lanes
    chunk = 512 if width % 512 == 0 else width
    share = team * tp_count // 2 * part
    piece = -(-ff // (team * 128)) * 128
    args = list(args)
    args[6] = head_gain.reshape(1, -1)
    args[9] = mix_gain.reshape(1, -1)
    vmem = pl.BlockSpec(memory_space=pltpu.VMEM)
    hbm = pl.BlockSpec(memory_space=pl.ANY)
    smem = pl.BlockSpec(memory_space=pltpu.SMEM)
    dma = pltpu.SemaphoreType.DMA
    in_specs = [vmem, hbm, vmem, hbm, hbm, smem, vmem, hbm, hbm, vmem, hbm, hbm, vmem, vmem, hbm]
    return pl.pallas_call(
        functools.partial(layer, sp_count, tp_count),
        out_shape=jax.ShapeDtypeStruct((part, width), bf16),
        in_specs=in_specs,
        out_specs=vmem,
        scratch_shapes=[
            pltpu.VMEM((sp_count * rows, 2 * q_a.shape[1] + vals.shape[1]), bf16),
            pltpu.VMEM((2, w_rows, ff), bf16),
            pltpu.VMEM((2, sp_count * w_rows, piece), bf16),
            pltpu.VMEM((piece, width), bf16),
            pltpu.VMEM(out_weight.shape, bf16),
            pltpu.VMEM((part, width), bf16),
            pltpu.VMEM((rows, vals.shape[1]), bf16),
            pltpu.VMEM((tp_count, part, width), bf16),
            pltpu.VMEM((tp_count, part, width), bf16),
            pltpu.VMEM((part, width), f32),
            pltpu.VMEM((team * (halo + rows), width), bf16),
            pltpu.VMEM((2, team * (halo + rows), piece), f32),
            pltpu.VMEM((team * rows, piece), bf16),
            pltpu.VMEM((width // chunk, 2, share, chunk), bf16),
            pltpu.VMEM((width // chunk, share, chunk), bf16),
            pltpu.VMEM((width // chunk, share, chunk), bf16),
            pltpu.VMEM((width // chunk, share, chunk), bf16),
            dma((10,)),
            dma((lines,)),
            dma((lines,)),
            dma((lines,)),
            dma((lines,)),
            dma((2, lines)),
            dma((2, lines)),
            dma((2, lines)),
            dma((2, lines)),
            dma((tp_count,)),
            dma((tp_count,)),
            dma((team, tp_count)),
            dma((team, tp_count)),
            dma((2,)),
            dma((team,)),
            dma((width // chunk,)),
            dma((width // chunk,)),
            dma((width // chunk, team * tp_count // 2)),
            dma((width // chunk, team * tp_count // 2)),
        ],
        compiler_params=pltpu.CompilerParams(
            collective_id=0, has_side_effects=True, vmem_limit_bytes=60 * 1024 * 1024
        ),
    )(*args)


def solution(mesh):
    in_specs = (
        P("sp", "tp"),
        P("sp", "tp"),
        P("sp", "tp"),
        P("sp", "tp"),
        P("sp", "tp"),
        P("tp"),
        P(),
        P("tp", None),
        P("sp", None),
        P(),
        P("sp", "tp"),
        P("sp", "tp"),
        P(None, "tp"),
        P(None, "tp"),
        P("tp", None),
    )
    body = functools.partial(shards, mesh.shape["sp"], mesh.shape["tp"])
    return jax.shard_map(
        body, mesh=mesh, in_specs=in_specs, out_specs=P(("sp", "tp"), None), check_vma=False
    )
```
